32 devices in a mesh: sp: 4 (over z), fs: 4 (over y, x), tp: 2 (over core).
Axes of the slice: x: 2, y: 2, z: 4, core: 2. Of those that a mesh axis runs over, the one named last changes fastest.
Arguments:
- inputs: bfloat16 [4, 1024, 2048], P('fs', ('sp', 'tp')), may hold values from -6 to 6
- norm_gain: float32 [2048], replicated, may hold values from 0.1 to 1.9
- w_glu_value: bfloat16 [2048, 1024], P(None, 'tp'), may hold values from -0.125 to 0.125
- w_glu_gate: bfloat16 [2048, 1024], P(None, 'tp'), may hold values from -0.125 to 0.125
- w_query_one: bfloat16 [2048, 512], P(None, 'tp'), may hold values from -2.5 to 2.5
- w_query_two: bfloat16 [2048, 512], P(None, 'tp'), may hold values from -2.5 to 2.5
- w_key_one: bfloat16 [2048, 512], P(None, 'tp'), may hold values from -2.5 to 2.5
- w_key_two: bfloat16 [2048, 512], P(None, 'tp'), may hold values from -2.5 to 2.5
- w_value: bfloat16 [2048, 1024], P(None, 'tp'), may hold values from -0.125 to 0.125
- conv_kernel: bfloat16 [31, 1024], P(None, 'tp'), may hold values from -1 to 1
- conv_gain: float32 [1024], P('tp'), may hold values from 0.1 to 1.9
- head_gain: float32 [128], replicated, may hold values from 0.1 to 1.9
- lambda_head: float32 [8], P('tp'), may hold values from 0.3 to 0.8
- w_out_conv: bfloat16 [1024, 2048], P('tp', 'fs'), may hold values from -0.125 to 0.125
- w_out_attn: bfloat16 [1024, 2048], P('tp', 'fs'), may hold values from -0.125 to 0.125
Outputs:
- mixed: bfloat16 [4, 1024, 2048], P('fs', ('sp', 'tp'))
- log_sums: float32 [4, 2, 8, 1024], P('fs', None, 'tp', 'sp')
The draws below stay inside these ranges and needn't reach their ends.
All inputs are finite; a program needn't handle non-finite values.
Results may differ from the reference program's by a relative error of at most 0.013.
Values may be sent and summed in bfloat16 or wider, within the bound.
A program may use at most 128 MiB of HBM per device.

```python
import jax
import jax.numpy as jnp
from jax import lax

D = 2048
DC = 1024
H = 8
KVH = 8
HD = 64
VD = 128
CW = 31
SEG = 64
SEQ = 1024
BATCH = 4
DA = 1024


def query_key_pair(key, which):
    base_key = jax.random.fold_in(key, 7 + which)
    spread = (3.0 / D) ** 0.5
    key_weight = jax.random.normal(jax.random.fold_in(base_key, 1), (D, KVH * HD), jnp.float32) * spread
    query_weight = jax.random.normal(jax.random.fold_in(base_key, 2), (D, H * HD), jnp.float32) * spread
    return (jnp.clip(query_weight, -2.5, 2.5), jnp.clip(key_weight, -2.5, 2.5))


def draw_w_query_one(key, part):
    return query_key_pair(key, 1)[0].astype(jnp.bfloat16)


def draw_w_key_one(key, part):
    return query_key_pair(key, 1)[1].astype(jnp.bfloat16)


def draw_w_query_two(key, part):
    return query_key_pair(key, 2)[0].astype(jnp.bfloat16)


def draw_w_key_two(key, part):
    return query_key_pair(key, 2)[1].astype(jnp.bfloat16)


def steps_of(key, extent, pieces, low, high):
    gain, own = 1.0, jax.random.fold_in(key, 6)
    for dim, parts in pieces:
        heights = jnp.exp(jax.random.uniform(jax.random.fold_in(own, dim), (parts,), jnp.float32, low / len(pieces), high / len(pieces)))
        gain = gain * jnp.repeat(heights, extent[dim] // parts).reshape([-1 if axis == dim else 1 for axis in range(len(extent))])
    return gain


def gaussian(stream_key, shape, scale, most, cuts=(), held_as=jnp.bfloat16):
    loudness = steps_of(stream_key, shape, cuts, -0.22, 0.18) if cuts else 1.0
    result = jax.random.normal(stream_key, shape, jnp.float32) * scale * loudness
    return jnp.minimum(jnp.maximum(result, -most), most).astype(held_as)


def setup_inputs(seed: int = 0) -> dict:
    streams_of = jax.random.split(jax.random.key(seed), 16)
    inputs = gaussian(streams_of[0], (BATCH, SEQ, D), 1.0, 6.0, ((0, 4), (1, 8)))
    norm_gain = jnp.clip(1.0 + 0.18 * jax.random.normal(streams_of[1], (D,), jnp.float32), 0.1, 1.9)
    w_glu_value = gaussian(streams_of[2], (D, DC), D ** -0.5, 0.125, ((1, 2),))
    w_glu_gate = gaussian(streams_of[3], (D, DC), D ** -0.5, 0.125, ((1, 2),))
    w_query_one = draw_w_query_one(jax.random.fold_in(streams_of[15], 71), 0)
    w_query_two = draw_w_query_two(jax.random.fold_in(streams_of[15], 71), 0)
    w_key_one = draw_w_key_one(jax.random.fold_in(streams_of[15], 71), 0)
    w_key_two = draw_w_key_two(jax.random.fold_in(streams_of[15], 71), 0)
    w_value = gaussian(streams_of[8], (D, KVH * VD), D ** -0.5, 0.125, ((1, 2),))
    conv_kernel = gaussian(streams_of[9], (CW, DC), CW ** -0.5, 1.0, ((1, 2),))
    conv_gain = jnp.clip(1.0 + 0.18 * jax.random.normal(streams_of[10], (DC,), jnp.float32), 0.1, 1.9)
    head_gain = jnp.clip(1.0 + 0.18 * jax.random.normal(streams_of[11], (VD,), jnp.float32), 0.1, 1.9)
    lambda_head = jnp.clip(0.3 + 0.5 * jax.random.uniform(streams_of[12], (H,), jnp.float32) ** steps_of(streams_of[12], (H,), ((0, 2),), -0.2, 0.2), 0.3, 0.8)
    w_out_conv = gaussian(streams_of[13], (DC, D), (DC + DA) ** -0.5, 0.125, ((0, 2), (1, 4)))
    w_out_attn = gaussian(streams_of[14], (DA, D), (DC + DA) ** -0.5, 0.125, ((0, 2), (1, 4)))
    return dict(inputs=inputs, norm_gain=norm_gain, w_glu_value=w_glu_value, w_glu_gate=w_glu_gate, w_query_one=w_query_one, w_query_two=w_query_two, w_key_one=w_key_one, w_key_two=w_key_two, w_value=w_value, conv_kernel=conv_kernel, conv_gain=conv_gain, head_gain=head_gain, lambda_head=lambda_head, w_out_conv=w_out_conv, w_out_attn=w_out_attn)


NEG_FILL = -1e+30
EPSILON = 1e-05
HEAD_SCALE = 0.8

def one_sequence(seq_rows, norm_gain, w_glu_value, w_glu_gate, w_query_one, w_query_two, w_key_one, w_key_two, w_value, conv_kernel, conv_gain, head_gain, lambda_head, w_out_conv, w_out_attn):
    rows_f = seq_rows.astype(jnp.float32)
    normed = (rows_f * lax.rsqrt(lax.optimization_barrier(jnp.mean(rows_f * rows_f, axis=-1, keepdims=True)) + EPSILON) * norm_gain).astype(jnp.bfloat16)

    def project(weight):
        return jnp.dot(normed, weight, preferred_element_type=jnp.float32).astype(jnp.bfloat16)
    glu_value = project(w_glu_value)
    glu_gate = project(w_glu_gate)
    query_one = project(w_query_one)
    query_two = project(w_query_two)
    key_one = project(w_key_one)
    key_two = project(w_key_two)
    values = project(w_value)
    gated = (glu_value.astype(jnp.float32) * jax.nn.sigmoid(glu_gate.astype(jnp.float32))).astype(jnp.bfloat16)
    extended = jnp.concatenate([jnp.zeros((CW - 1, DC), jnp.bfloat16), gated], axis=0).astype(jnp.float32)
    kernel_f = conv_kernel.astype(jnp.float32)
    convolved = jnp.zeros((SEQ, DC), jnp.float32)
    for tap_index in range(CW):
        convolved = convolved + kernel_f[tap_index][None, :] * extended[tap_index:tap_index + SEQ]
    row_mean = lax.optimization_barrier(jnp.mean(convolved, axis=-1, keepdims=True))
    row_square = lax.optimization_barrier(jnp.mean(convolved * convolved, axis=-1, keepdims=True))
    conv_out = jax.nn.silu((convolved - row_mean) * lax.rsqrt(row_square - row_mean * row_mean + EPSILON) * conv_gain).astype(jnp.bfloat16)
    group = H // KVH
    query_one_r = query_one.reshape(SEQ, KVH, group, HD).astype(jnp.float32)
    query_two_r = query_two.reshape(SEQ, KVH, group, HD).astype(jnp.float32)
    key_one_r = key_one.reshape(SEQ, KVH, HD).astype(jnp.float32)
    key_two_r = key_two.reshape(SEQ, KVH, HD).astype(jnp.float32)
    values_r = values.reshape(SEQ, KVH, VD).astype(jnp.float32)
    lambda_r = lambda_head.reshape(KVH, group)
    score_scale = HD ** (-0.5)
    block_rows = min(512, SEQ)
    attn_blocks = []
    log_blocks = []
    for block_start in range(0, SEQ, block_rows):
        block_end = min(block_start + block_rows, SEQ)
        query_pos = jnp.arange(block_start, block_end, dtype=jnp.int32)
        key_pos = jnp.arange(0, block_end, dtype=jnp.int32)
        allowed = ((key_pos // SEG)[None, :] <= (query_pos // SEG)[:, None])[:, None, None, :]
        pooled_list = []
        log_list = []
        for queries, key_rows in ((query_one_r, key_one_r), (query_two_r, key_two_r)):
            scores = jnp.einsum('tgrd,kgd->tgrk', queries[block_start:block_end], key_rows[:block_end]) * score_scale
            scores = jnp.where(allowed, scores, NEG_FILL)
            row_max = lax.optimization_barrier(jnp.max(scores, axis=-1))
            weights = jnp.where(allowed, jnp.exp(scores - row_max[..., None]), 0.0)
            weight_sum = lax.optimization_barrier(jnp.sum(weights, axis=-1))
            log_list.append(row_max + jnp.log(weight_sum))
            pooled = jnp.einsum('tgrk,kgv->tgrv', weights.astype(jnp.bfloat16).astype(jnp.float32), values_r[:block_end])
            pooled_list.append(pooled / weight_sum[..., None])
        head_out = pooled_list[0] - lambda_r[None, :, :, None] * pooled_list[1]
        head_out = head_out * lax.rsqrt(lax.optimization_barrier(jnp.mean(head_out * head_out, axis=-1, keepdims=True)) + EPSILON) * head_gain * HEAD_SCALE
        attn_blocks.append(head_out.astype(jnp.bfloat16).reshape(block_end - block_start, H * VD))
        log_blocks.append(jnp.stack(log_list, axis=0).reshape(2, block_end - block_start, H))
    attn_out = jnp.concatenate(attn_blocks, axis=0)
    log_sums = jnp.transpose(jnp.concatenate(log_blocks, axis=1), (0, 2, 1))
    mixed = jnp.dot(conv_out, w_out_conv, preferred_element_type=jnp.float32) + jnp.dot(attn_out, w_out_attn, preferred_element_type=jnp.float32)
    return (mixed.astype(jnp.bfloat16), log_sums)

def reference(inputs, norm_gain, w_glu_value, w_glu_gate, w_query_one, w_query_two, w_key_one, w_key_two, w_value, conv_kernel, conv_gain, head_gain, lambda_head, w_out_conv, w_out_attn):

    def per_sequence(seq_rows):
        return one_sequence(seq_rows, norm_gain, w_glu_value, w_glu_gate, w_query_one, w_query_two, w_key_one, w_key_two, w_value, conv_kernel, conv_gain, head_gain, lambda_head, w_out_conv, w_out_attn)
    mixed, log_sums = lax.map(per_sequence, inputs)
    return (mixed, log_sums)
```

```python
import functools

import jax
import jax.numpy as jnp
from jax import lax
from jax.experimental import pallas as pl
from jax.experimental.pallas import tpu as pltpu
from jax.sharding import PartitionSpec as P

HD = 64
VD = 128
SEG = 64
TILE = 256

NEG_FILL = -1e30
EPSILON = 1e-05
HEAD_SCALE = 0.8
MESH = pl.DeviceIdType.MESH


def kernel(
    n_sp,
    n_fs,
    tiles,
    channels,
    x_hbm,
    wgv,
    wgg,
    wq1,
    wq2,
    wk1,
    wk2,
    wv,
    woc,
    woa,
    norm_gain,
    conv_kernel,
    conv_gain,
    head_gain,
    lambda_head,
    mixed,
    logs,
    xb,
    nb,
    wall,
    wout,
    pbuf,
    gbuf,
    halo,
    ext,
    taps,
    cbuf,
    stat,
    stat_in,
    qm,
    bias,
    acc,
    m_sc,
    l_sc,
    act,
    part_out,
    part_in,
    own,
    x_sem,
    w_sem,
    wl_sem,
    wo_send,
    wo_recv,
    right_send,
    left_recv,
    pair_send,
    pair_recv,
    halo_send,
    halo_recv,
    stat_send,
    stat_recv,
    out_send,
    out_recv,
):
    sp = lax.axis_index("sp")
    fs = lax.axis_index("fs")
    tp = lax.axis_index("tp")
    other = 1 - tp
    half = xb.shape[0]
    rows = 2 * half
    t_glu, t_qk = tiles
    conv_tiles = t_glu
    base_q1 = 2 * t_glu
    base_q2 = base_q1 + t_qk
    base_k1 = base_q2 + t_qk
    base_k2 = base_k1 + t_qk
    base_v = base_k2 + t_qk
    n_tiles = wall.shape[0]
    heads = t_qk * TILE // HD
    width = wgv.shape[1]
    lanes = width // 128

    x_copy = pltpu.make_async_copy(x_hbm.at[0], xb, x_sem)
    x_copy.start()
    w_copies = []
    for ref, base, count in (
        (wgv, 0, t_glu),
        (wgg, t_glu, t_glu),
        (wq1, base_q1, t_qk),
        (wq2, base_q2, t_qk),
        (wk1, base_k1, t_qk),
        (wk2, base_k2, t_qk),
        (wv, base_v, n_tiles - base_v),
    ):
        for t in range(count):
            copy = pltpu.make_async_copy(
                ref.at[:, pl.ds(t * TILE, TILE)], wall.at[base + t], w_sem.at[base + t]
            )
            copy.start()
            w_copies.append(copy)
    depth = woc.shape[0]
    wo_local = [
        pltpu.make_async_copy(ref, wout.at[fs, pl.ds(which * depth, depth)], wl_sem.at[which])
        for which, ref in enumerate((woc, woa))
    ]

    barrier = pltpu.get_barrier_semaphore()

    def greet(**where):
        pl.semaphore_signal(barrier, inc=1, device_id=where, device_id_type=MESH)

    greet(tp=other)
    for d in range(1, n_fs):
        greet(fs=lax.rem(fs + d, n_fs))

    @pl.when(sp > 0)
    def _():
        greet(sp=sp - 1)

    @pl.when(sp < n_sp - 1)
    def _():
        greet(sp=sp + 1)

    x_copy.wait()
    gain = norm_gain[...]

    def norm_rows(r, carry):
        at = pl.ds(pl.multiple_of(r * 16, 16), 16)
        x = xb[at, :].astype(jnp.float32)
        scale = lax.rsqrt(jnp.mean(x * x, axis=-1, keepdims=True) + EPSILON)
        nb[0, tp, at, :] = (x * scale * gain).astype(jnp.bfloat16)
        return carry

    lax.fori_loop(0, half // 16, norm_rows, 0)

    at_end = (sp == 0) | (sp == n_sp - 1)

    @pl.when(at_end)
    def _():
        pl.semaphore_wait(barrier, n_fs + 1)

    @pl.when(jnp.logical_not(at_end))
    def _():
        pl.semaphore_wait(barrier, n_fs + 2)

    def to_right(s):
        return pltpu.make_async_remote_copy(
            nb.at[s, tp],
            nb.at[s + 1, tp],
            right_send.at[s],
            left_recv.at[s + 1],
            device_id={"sp": lax.rem(sp + 1, n_sp)},
            device_id_type=MESH,
        )

    def to_pair(s):
        return pltpu.make_async_remote_copy(
            nb.at[s, tp],
            nb.at[s, tp],
            pair_send.at[s],
            pair_recv.at[s],
            device_id={"tp": other},
            device_id_type=MESH,
        )

    def from_pair(s):
        return pltpu.make_async_remote_copy(
            nb.at[s, other],
            nb.at[s, other],
            pair_send.at[s],
            pair_recv.at[s],
            device_id={"tp": other},
            device_id_type=MESH,
        )

    def weights_to(d, which):
        ref = (woc, woa)[which]
        return pltpu.make_async_remote_copy(
            ref,
            wout.at[fs, pl.ds(which * depth, depth)],
            wo_send.at[d, which],
            wo_recv.at[fs, which],
            device_id={"fs": lax.rem(fs + d, n_fs)},
            device_id_type=MESH,
        )

    def weights_from(d, which):
        source = lax.rem(fs + d, n_fs)
        return pltpu.make_async_remote_copy(
            wout.at[source, pl.ds(which * depth, depth)],
            wout.at[source, pl.ds(which * depth, depth)],
            wo_send.at[d, which],
            wo_recv.at[source, which],
            device_id={"fs": source},
            device_id_type=MESH,
        )

    to_pair(0).start()

    @pl.when(sp < n_sp - 1)
    def _():
        to_right(0).start()

    for which in range(2):
        for d in range(1, n_fs):
            weights_to(d, which).start()
    for copy in wo_local:
        copy.start()

    key_seg = lax.broadcasted_iota(jnp.int32, (rows, rows), 0) // SEG
    query_seg = lax.broadcasted_iota(jnp.int32, (rows, rows), 1) // SEG
    bias[...] = jnp.where(key_seg <= query_seg, 0.0, NEG_FILL)
    m_sc[...] = jnp.full(m_sc.shape, NEG_FILL, jnp.float32)
    l_sc[...] = jnp.zeros(l_sc.shape, jnp.float32)
    acc[...] = jnp.zeros(acc.shape, jnp.float32)
    n_taps = conv_kernel.shape[0]
    taps_f = conv_kernel[...].astype(jnp.float32)
    for c in range(lanes):
        taps[c, 0:n_taps, :] = taps_f[:, c * 128 : (c + 1) * 128]

    from_pair(0).wait_recv()

    def project(s, t):
        block = nb[s].reshape(rows, nb.shape[3])
        pbuf[t] = jnp.dot(block, wall[t], preferred_element_type=jnp.float32).astype(jnp.bfloat16)

    def first_project(t, carry):
        pltpu.make_async_copy(
            wgv.at[:, pl.ds(0, TILE)], wall.at[t], w_sem.at[t]
        ).wait()
        project(0, t)
        return carry

    lax.fori_loop(0, base_q1, first_project, 0)
    for t in range(conv_tiles):
        value = pbuf[t].astype(jnp.float32)
        gate = pbuf[conv_tiles + t].astype(jnp.float32)
        gbuf[:, t * TILE : (t + 1) * TILE] = (value * jax.nn.sigmoid(gate)).astype(jnp.bfloat16)
    reach = halo.shape[0]
    halo_copy = pltpu.make_async_remote_copy(
        gbuf.at[pl.ds(rows - reach, reach)],
        halo,
        halo_send,
        halo_recv,
        device_id={"sp": lax.rem(sp + 1, n_sp)},
        device_id_type=MESH,
    )

    @pl.when(sp < n_sp - 1)
    def _():
        halo_copy.start()

    lax.fori_loop(base_q1, n_tiles, first_project, 0)
    lane = lax.broadcasted_iota(jnp.int32, (rows, 128), 1)
    for i, base in enumerate((base_q1, base_q2)):
        for h in range(heads):
            tile, start = divmod(h * HD, TILE)
            start = start // 128 * 128
            queries = pbuf[base + tile, :, start : start + 128].astype(jnp.float32)
            inside = (lane // HD) == (h * HD % 128) // HD
            qm[i * heads + h] = jnp.where(inside, queries * HD**-0.5, 0.0).astype(jnp.bfloat16)

    for c in range(lanes):
        ext[c, reach:, :] = gbuf[:, c * 128 : (c + 1) * 128].astype(jnp.float32)

    @pl.when(sp == 0)
    def _():
        halo[...] = jnp.zeros(halo.shape, halo.dtype)

    @pl.when(sp > 0)
    def _():
        halo_copy.wait_recv()

    for c in range(lanes):
        ext[c, 0:reach, :] = halo[:, c * 128 : (c + 1) * 128].astype(jnp.float32)

    def conv_lanes(c, carry):
        sums, squares = carry
        lead = reach - (n_taps - 1)
        total = jnp.zeros((rows, 128), jnp.float32)
        for j in range(n_taps):
            total = total + taps[c, j : j + 1, :] * ext[c, lead + j : lead + j + rows, :]
        cbuf[c] = total
        return sums + total, squares + total * total

    zero = jnp.zeros((rows, 128), jnp.float32)
    sums, squares = lax.fori_loop(0, lanes, conv_lanes, (zero, zero))
    stat[...] = jnp.where(
        lane == 0,
        jnp.sum(sums, axis=-1, keepdims=True),
        jnp.sum(squares, axis=-1, keepdims=True),
    )
    stat_copy = pltpu.make_async_remote_copy(
        stat, stat_in, stat_send, stat_recv, device_id={"tp": other}, device_id_type=MESH
    )
    stat_copy.start()

    def take_next(s):
        to_right(s).wait_recv()

        @pl.when(sp < n_sp - 1)
        def _():
            to_right(s + 1).start()

        to_pair(s + 1).start()

    def step(s, carry):
        @pl.when((sp < n_sp - 1) & (s < sp))
        def _():
            take_next(s)

        @pl.when(s > 0)
        def _():
            from_pair(s).wait_recv()

            def again(t, inner):
                project(s, t)
                return inner

            lax.fori_loop(base_k1, n_tiles, again, 0)

            @pl.when(s == 1)
            def _():
                bias[...] = jnp.zeros(bias.shape, jnp.float32)

        for h in range(heads):
            v_tile, v_start = divmod(h * VD, TILE)
            values = pbuf[base_v + v_tile, :, v_start : v_start + VD]
            tile, start = divmod(h * HD, TILE)
            start = start // 128 * 128
            for i, base in enumerate((base_k1, base_k2)):
                c = i * heads + h
                keys = pbuf[base + tile, :, start : start + 128]
                scores = lax.dot_general(
                    keys, qm[c], (((1,), (1,)), ((), ())), preferred_element_type=jnp.float32
                )
                scores = scores + bias[...]
                old = m_sc[c : c + 1, :]
                new = jnp.maximum(old, jnp.max(scores, axis=0, keepdims=True))
                weights = jnp.exp(scores - new)
                factor = jnp.exp(old - new)
                m_sc[c : c + 1, :] = new
                l_sc[c : c + 1, :] = l_sc[c : c + 1, :] * factor + jnp.sum(
                    weights, axis=0, keepdims=True
                )
                acc[c] = acc[c] * factor + lax.dot_general(
                    values,
                    weights.astype(jnp.bfloat16),
                    (((0,), (0,)), ((), ())),
                    preferred_element_type=jnp.float32,
                )

        @pl.when((sp == n_sp - 1) & (s < sp))
        def _():
            take_next(s)

        return carry

    stat_copy.wait_recv()
    both = stat[...] + stat_in[...]
    row_mean = both[:, 0:1] / channels
    row_square = both[:, 1:2] / channels
    row_scale = lax.rsqrt(row_square - row_mean * row_mean + EPSILON)
    for c in range(lanes):
        at = slice(c * 128, (c + 1) * 128)
        z = (cbuf[c] - row_mean) * row_scale * conv_gain[:, at]
        act[:, at] = jax.nn.silu(z).astype(jnp.bfloat16)

    lax.fori_loop(0, sp + 1, step, 0)

    logs[...] = m_sc[...] + jnp.log(l_sc[...])
    for h in range(heads):
        one = acc[h] / l_sc[h : h + 1, :]
        two = acc[heads + h] / l_sc[heads + h : heads + h + 1, :]
        head_out = one - lambda_head[h] * two
        head_out = head_out * lax.rsqrt(
            jnp.mean(head_out * head_out, axis=0, keepdims=True) + EPSILON
        )
        head_out = head_out.T * head_gain[...] * HEAD_SCALE
        act[:, width + h * VD : width + (h + 1) * VD] = head_out.astype(jnp.bfloat16)

    for copy in wo_local:
        copy.wait()
    for d in range(1, n_fs):
        for which in range(2):
            weights_from(d, which).wait_recv()

    def give(f):
        return pltpu.make_async_remote_copy(
            part_out.at[f],
            part_in.at[f],
            out_send.at[f],
            out_recv.at[f],
            device_id={"tp": other},
            device_id_type=MESH,
        )

    def columns(f, carry):
        theirs = act[pl.ds(pl.multiple_of(other * half, half), half), :]
        part_out[f] = jnp.dot(theirs, wout[f], preferred_element_type=jnp.float32).astype(
            jnp.bfloat16
        )
        give(f).start()
        mine = act[pl.ds(pl.multiple_of(tp * half, half), half), :]
        own[f] = jnp.dot(mine, wout[f], preferred_element_type=jnp.float32)
        return carry

    lax.fori_loop(0, n_fs, columns, 0)
    span = wout.shape[2]
    for f in range(n_fs):
        give(f).wait_recv()
        mixed[0, :, f * span : (f + 1) * span] = (
            own[f] + part_in[f].astype(jnp.float32)
        ).astype(jnp.bfloat16)

    def sent(s, carry):
        to_pair(s).wait_send()

        @pl.when(sp < n_sp - 1)
        def _():
            to_right(s).wait_send()

        return carry

    lax.fori_loop(0, sp + 1, sent, 0)

    @pl.when(sp < n_sp - 1)
    def _():
        halo_copy.wait_send()

    stat_copy.wait_send()
    for d in range(1, n_fs):
        for which in range(2):
            weights_to(d, which).wait_send()
    for f in range(n_fs):
        give(f).wait_send()


def body(
    n_sp,
    n_fs,
    inputs,
    norm_gain,
    w_glu_value,
    w_glu_gate,
    w_query_one,
    w_query_two,
    w_key_one,
    w_key_two,
    w_value,
    conv_kernel,
    conv_gain,
    head_gain,
    lambda_head,
    w_out_conv,
    w_out_attn,
):
    half, model = inputs.shape[1:]
    rows = 2 * half
    width = w_glu_value.shape[1]
    t_glu = width // TILE
    t_qk = w_query_one.shape[1] // TILE
    t_v = w_value.shape[1] // TILE
    n_tiles = 2 * t_glu + 4 * t_qk + t_v
    heads = w_query_one.shape[1] // HD
    lanes = width // 128
    depth, span = w_out_conv.shape
    reach = -(-(conv_kernel.shape[0] - 1) // 16) * 16
    hbm = pl.BlockSpec(memory_space=pl.ANY)
    vmem = pl.BlockSpec(memory_space=pltpu.VMEM)
    f32, bf16 = jnp.float32, jnp.bfloat16
    dma = pltpu.SemaphoreType.DMA
    mixed, logs = pl.pallas_call(
        functools.partial(kernel, n_sp, n_fs, (t_glu, t_qk), 2 * width),
        out_shape=(
            jax.ShapeDtypeStruct((1, half, model), bf16),
            jax.ShapeDtypeStruct((2 * heads, rows), f32),
        ),
        in_specs=[hbm] * 10 + [vmem] * 4 + [pl.BlockSpec(memory_space=pltpu.SMEM)],
        out_specs=(vmem, vmem),
        scratch_shapes=[
            pltpu.VMEM((half, model), bf16),
            pltpu.VMEM((n_sp, 2, half, model), bf16),
            pltpu.VMEM((n_tiles, model, TILE), bf16),
            pltpu.VMEM((n_fs, 2 * depth, span), bf16),
            pltpu.VMEM((n_tiles, rows, TILE), bf16),
            pltpu.VMEM((rows, width), bf16),
            pltpu.VMEM((reach, width), bf16),
            pltpu.VMEM((lanes, reach + rows, 128), f32),
            pltpu.VMEM((lanes, reach, 128), f32),
            pltpu.VMEM((lanes, rows, 128), f32),
            pltpu.VMEM((rows, 128), f32),
            pltpu.VMEM((rows, 128), f32),
            pltpu.VMEM((2 * heads, rows, 128), bf16),
            pltpu.VMEM((rows, rows), f32),
            pltpu.VMEM((2 * heads, VD, rows), f32),
            pltpu.VMEM((2 * heads, rows), f32),
            pltpu.VMEM((2 * heads, rows), f32),
            pltpu.VMEM((rows, width + heads * VD), bf16),
            pltpu.VMEM((n_fs, half, span), bf16),
            pltpu.VMEM((n_fs, half, span), bf16),
            pltpu.VMEM((n_fs, half, span), f32),
            dma,
            dma((n_tiles,)),
            dma((2,)),
            dma((n_fs, 2)),
            dma((n_fs, 2)),
            dma((n_sp,)),
            dma((n_sp,)),
            dma((n_sp,)),
            dma((n_sp,)),
            dma,
            dma,
            dma,
            dma,
            dma((n_fs,)),
            dma((n_fs,)),
        ],
        compiler_params=pltpu.CompilerParams(
            collective_id=0, has_side_effects=True, vmem_limit_bytes=63 * 1024 * 1024
        ),
        name="layer",
    )(
        inputs,
        w_glu_value,
        w_glu_gate,
        w_query_one,
        w_query_two,
        w_key_one,
        w_key_two,
        w_value,
        w_out_conv,
        w_out_attn,
        norm_gain.reshape(1, model),
        conv_kernel,
        conv_gain.reshape(1, width),
        head_gain.reshape(1, VD),
        lambda_head,
    )
    return mixed, logs.reshape(1, 2, heads, rows)


def solution(mesh):
    return jax.shard_map(
        functools.partial(body, mesh.shape["sp"], mesh.shape["fs"]),
        mesh=mesh,
        in_specs=(
            P("fs", ("sp", "tp"), None),
            P(),
            P(None, "tp"),
            P(None, "tp"),
            P(None, "tp"),
            P(None, "tp"),
            P(None, "tp"),
            P(None, "tp"),
            P(None, "tp"),
            P(None, "tp"),
            P("tp"),
            P(),
            P("tp"),
            P("tp", "fs"),
            P("tp", "fs"),
        ),
        out_specs=(P("fs", ("sp", "tp"), None), P("fs", None, "tp", "sp")),
        check_vma=False,
    )
```

```python
import functools

import jax
import jax.numpy as jnp
from jax import lax
from jax.experimental import pallas as pl
from jax.experimental.pallas import tpu as pltpu
from jax.sharding import PartitionSpec as P

HD = 64
VD = 128
SEG = 64
TILE = 256

NEG_FILL = -1e30
EPSILON = 1e-05
HEAD_SCALE = 0.8
MESH = pl.DeviceIdType.MESH


def kernel(
    n_sp,
    n_fs,
    tiles,
    channels,
    x_hbm,
    wgv,
    wgg,
    wq1,
    wq2,
    wk1,
    wk2,
    wv,
    woc,
    woa,
    norm_gain,
    conv_kernel,
    conv_gain,
    head_gain,
    lambda_head,
    own,
    part_in,
    max_out,
    sum_out,
    xb,
    nb,
    wall,
    wout,
    pbuf,
    gbuf,
    halo,
    ext,
    taps,
    cbuf,
    stat,
    stat_in,
    qm,
    bias,
    acc,
    m_sc,
    l_sc,
    act,
    part_out,
    x_sem,
    w_sem,
    wl_sem,
    wo_send,
    wo_recv,
    right_send,
    left_recv,
    pair_send,
    pair_recv,
    halo_send,
    halo_recv,
    stat_send,
    stat_recv,
    out_send,
    out_recv,
):
    sp = lax.axis_index("sp")
    fs = lax.axis_index("fs")
    tp = lax.axis_index("tp")
    other = 1 - tp
    half = xb.shape[0]
    rows = 2 * half
    t_glu, t_qk = tiles
    conv_tiles = t_glu
    base_q1 = 2 * t_glu
    base_q2 = base_q1 + t_qk
    base_k1 = base_q2 + t_qk
    base_k2 = base_k1 + t_qk
    base_v = base_k2 + t_qk
    n_tiles = wall.shape[0]
    heads = t_qk * TILE // HD
    width = wgv.shape[1]
    lanes = width // 128

    x_copy = pltpu.make_async_copy(x_hbm.at[0], xb, x_sem)
    x_copy.start()
    w_copies = []
    for ref, base, count in (
        (wgv, 0, t_glu),
        (wgg, t_glu, t_glu),
        (wq1, base_q1, t_qk),
        (wq2, base_q2, t_qk),
        (wk1, base_k1, t_qk),
        (wk2, base_k2, t_qk),
        (wv, base_v, n_tiles - base_v),
    ):
        for t in range(count):
            copy = pltpu.make_async_copy(
                ref.at[:, pl.ds(t * TILE, TILE)], wall.at[base + t], w_sem.at[base + t]
            )
            copy.start()
            w_copies.append(copy)
    depth = woc.shape[0]
    wo_local = [
        pltpu.make_async_copy(ref, wout.at[fs, pl.ds(which * depth, depth)], wl_sem.at[which])
        for which, ref in enumerate((woc, woa))
    ]

    barrier = pltpu.get_barrier_semaphore()

    def greet(**where):
        pl.semaphore_signal(barrier, inc=1, device_id=where, device_id_type=MESH)

    greet(tp=other)
    for d in range(1, n_fs):
        greet(fs=lax.rem(fs + d, n_fs))

    @pl.when(sp > 0)
    def _():
        greet(sp=sp - 1)

    @pl.when(sp < n_sp - 1)
    def _():
        greet(sp=sp + 1)

    x_copy.wait()
    gain = norm_gain[...]

    def norm_rows(r, carry):
        at = pl.ds(pl.multiple_of(r * 16, 16), 16)
        x = xb[at, :].astype(jnp.float32)
        scale = lax.rsqrt(jnp.mean(x * x, axis=-1, keepdims=True) + EPSILON)
        nb[0, tp, at, :] = (x * scale * gain).astype(jnp.bfloat16)
        return carry

    lax.fori_loop(0, half // 16, norm_rows, 0)

    at_end = (sp == 0) | (sp == n_sp - 1)

    @pl.when(at_end)
    def _():
        pl.semaphore_wait(barrier, n_fs + 1)

    @pl.when(jnp.logical_not(at_end))
    def _():
        pl.semaphore_wait(barrier, n_fs + 2)

    def to_right(s):
        return pltpu.make_async_remote_copy(
            nb.at[s, tp],
            nb.at[s + 1, tp],
            right_send.at[s],
            left_recv.at[s + 1],
            device_id={"sp": lax.rem(sp + 1, n_sp)},
            device_id_type=MESH,
        )

    def to_pair(s):
        return pltpu.make_async_remote_copy(
            nb.at[s, tp],
            nb.at[s, tp],
            pair_send.at[s],
            pair_recv.at[s],
            device_id={"tp": other},
            device_id_type=MESH,
        )

    def from_pair(s):
        return pltpu.make_async_remote_copy(
            nb.at[s, other],
            nb.at[s, other],
            pair_send.at[s],
            pair_recv.at[s],
            device_id={"tp": other},
            device_id_type=MESH,
        )

    def place(index):
        if n_fs % 2:
            return index
        pair = index // 2
        return pair * 2 + lax.rem(lax.rem(index, 2) + pair, 2)

    seat = place(fs)

    def owner(d):
        return place(lax.rem(seat + n_fs + d, n_fs))

    def halves(d):
        if 2 * abs(d) < n_fs:
            return (0, 1) if d > 0 else (1, 0)
        if 2 * abs(d) == n_fs:
            return (0,) if d > 0 else (1,)
        return ()

    def weights_pass(d, which):
        sign = 1 if d > 0 else -1
        source = owner(-(d - sign))
        there = wout.at[source, pl.ds(which * depth, depth)]
        return pltpu.make_async_remote_copy(
            (woc, woa)[which] if abs(d) == 1 else there,
            there,
            wo_send.at[d + n_fs, which],
            wo_recv.at[source, which],
            device_id={"fs": owner(sign)},
            device_id_type=MESH,
        )

    def weights_from(d, which):
        source = owner(-d)
        there = wout.at[source, pl.ds(which * depth, depth)]
        return pltpu.make_async_remote_copy(
            there,
            there,
            wo_send.at[d + n_fs, which],
            wo_recv.at[source, which],
            device_id={"fs": source},
            device_id_type=MESH,
        )

    ways = [d for m in range(1, n_fs // 2 + 1) for d in (m, -m)]

    to_pair(0).start()

    @pl.when(sp < n_sp - 1)
    def _():
        to_right(0).start()

    for which in range(2):
        for d in ways[:2]:
            if which < len(halves(d)):
                weights_pass(d, halves(d)[which]).start()
    for copy in wo_local:
        copy.start()

    key_seg = lax.broadcasted_iota(jnp.int32, (rows, rows), 0) // SEG
    query_seg = lax.broadcasted_iota(jnp.int32, (rows, rows), 1) // SEG
    bias[...] = jnp.where(key_seg <= query_seg, 0.0, NEG_FILL)
    m_sc[...] = jnp.full(m_sc.shape, NEG_FILL, jnp.float32)
    l_sc[...] = jnp.zeros(l_sc.shape, jnp.float32)
    acc[...] = jnp.zeros(acc.shape, jnp.float32)
    n_taps = conv_kernel.shape[0]
    taps_f = conv_kernel[...].astype(jnp.float32)
    for c in range(lanes):
        taps[c, 0:n_taps, :] = taps_f[:, c * 128 : (c + 1) * 128]

    from_pair(0).wait_recv()

    def project(s, t):
        block = nb[s].reshape(rows, nb.shape[3])
        pbuf[t] = jnp.dot(block, wall[t], preferred_element_type=jnp.float32).astype(jnp.bfloat16)

    def first_project(t, carry):
        pltpu.make_async_copy(
            wgv.at[:, pl.ds(0, TILE)], wall.at[t], w_sem.at[t]
        ).wait()
        project(0, t)
        return carry

    lax.fori_loop(0, base_q1, first_project, 0)
    for t in range(conv_tiles):
        value = pbuf[t].astype(jnp.float32)
        gate = pbuf[conv_tiles + t].astype(jnp.float32)
        gbuf[:, t * TILE : (t + 1) * TILE] = (value * jax.nn.sigmoid(gate)).astype(jnp.bfloat16)
    reach = halo.shape[0]
    halo_copy = pltpu.make_async_remote_copy(
        gbuf.at[pl.ds(rows - reach, reach)],
        halo,
        halo_send,
        halo_recv,
        device_id={"sp": lax.rem(sp + 1, n_sp)},
        device_id_type=MESH,
    )

    @pl.when(sp < n_sp - 1)
    def _():
        halo_copy.start()

    lax.fori_loop(base_q1, n_tiles, first_project, 0)
    lane = lax.broadcasted_iota(jnp.int32, (rows, 128), 1)
    for i, base in enumerate((base_q1, base_q2)):
        for h in range(heads):
            tile, start = divmod(h * HD, TILE)
            start = start // 128 * 128
            queries = pbuf[base + tile, :, start : start + 128].astype(jnp.float32)
            inside = (lane // HD) == (h * HD % 128) // HD
            qm[i * heads + h] = jnp.where(inside, queries * HD**-0.5, 0.0).astype(jnp.bfloat16)

    for c in range(lanes):
        ext[c, reach:, :] = gbuf[:, c * 128 : (c + 1) * 128].astype(jnp.float32)

    @pl.when(sp == 0)
    def _():
        halo[...] = jnp.zeros(halo.shape, halo.dtype)

    @pl.when(sp > 0)
    def _():
        halo_copy.wait_recv()

    for c in range(lanes):
        ext[c, 0:reach, :] = halo[:, c * 128 : (c + 1) * 128].astype(jnp.float32)

    def conv_lanes(c, carry):
        sums, squares = carry
        lead = reach - (n_taps - 1)
        total = jnp.zeros((rows, 128), jnp.float32)
        for j in range(n_taps):
            total = total + taps[c, j : j + 1, :] * ext[c, lead + j : lead + j + rows, :]
        cbuf[c] = total
        return sums + total, squares + total * total

    zero = jnp.zeros((rows, 128), jnp.float32)
    sums, squares = lax.fori_loop(0, lanes, conv_lanes, (zero, zero))
    stat[...] = jnp.where(
        lane == 0,
        jnp.sum(sums, axis=-1, keepdims=True),
        jnp.sum(squares, axis=-1, keepdims=True),
    )
    stat_copy = pltpu.make_async_remote_copy(
        stat, stat_in, stat_send, stat_recv, device_id={"tp": other}, device_id_type=MESH
    )
    stat_copy.start()

    def take_next(s):
        to_right(s).wait_recv()

        @pl.when(sp < n_sp - 1)
        def _():
            to_right(s + 1).start()

        to_pair(s + 1).start()

    def step(s, carry):
        @pl.when((sp < n_sp - 1) & (s < sp))
        def _():
            take_next(s)

        @pl.when(s > 0)
        def _():
            from_pair(s).wait_recv()

            def again(t, inner):
                project(s, t)
                return inner

            lax.fori_loop(base_k1, n_tiles, again, 0)

            @pl.when(s == 1)
            def _():
                bias[...] = jnp.zeros(bias.shape, jnp.float32)

        for h in range(heads):
            v_tile, v_start = divmod(h * VD, TILE)
            values = pbuf[base_v + v_tile, :, v_start : v_start + VD]
            tile, start = divmod(h * HD, TILE)
            start = start // 128 * 128
            for i, base in enumerate((base_k1, base_k2)):
                c = i * heads + h
                keys = pbuf[base + tile, :, start : start + 128]
                scores = lax.dot_general(
                    keys, qm[c], (((1,), (1,)), ((), ())), preferred_element_type=jnp.float32
                )
                scores = scores + bias[...]
                old = m_sc[c : c + 1, :]
                new = jnp.maximum(old, jnp.max(scores, axis=0, keepdims=True))
                weights = jnp.exp(scores - new)
                factor = jnp.exp(old - new)
                m_sc[c : c + 1, :] = new
                l_sc[c : c + 1, :] = l_sc[c : c + 1, :] * factor + jnp.sum(
                    weights, axis=0, keepdims=True
                )
                acc[c] = acc[c] * factor + lax.dot_general(
                    values,
                    weights.astype(jnp.bfloat16),
                    (((0,), (0,)), ((), ())),
                    preferred_element_type=jnp.float32,
                )

        @pl.when(s == 0)
        def _():
            for d in ways[2:]:
                for which in halves(d):
                    weights_from(d - (1 if d > 0 else -1), which).wait_recv()
                    weights_pass(d, which).start()

        @pl.when((sp == n_sp - 1) & (s < sp))
        def _():
            take_next(s)

        return carry

    stat_copy.wait_recv()
    both = stat[...] + stat_in[...]
    row_mean = both[:, 0:1] / channels
    row_square = both[:, 1:2] / channels
    row_scale = lax.rsqrt(row_square - row_mean * row_mean + EPSILON)
    for c in range(lanes):
        at = slice(c * 128, (c + 1) * 128)
        z = (cbuf[c] - row_mean) * row_scale * conv_gain[:, at]
        act[:, at] = jax.nn.silu(z).astype(jnp.bfloat16)

    lax.fori_loop(0, sp + 1, step, 0)

    for i in range(2):
        max_out[0, i] = m_sc[i * heads : (i + 1) * heads, :]
        sum_out[0, i] = l_sc[i * heads : (i + 1) * heads, :]
    for h in range(heads):
        one = acc[h] / l_sc[h : h + 1, :]
        two = acc[heads + h] / l_sc[heads + h : heads + h + 1, :]
        head_out = one - lambda_head[h] * two
        head_out = head_out * lax.rsqrt(
            jnp.mean(head_out * head_out, axis=0, keepdims=True) + EPSILON
        )
        head_out = head_out.T * head_gain[...] * HEAD_SCALE
        act[:, width + h * VD : width + (h + 1) * VD] = head_out.astype(jnp.bfloat16)

    for copy in wo_local:
        copy.wait()
    passed = [(d - (1 if d > 0 else -1), which) for d in ways[2:] for which in halves(d)]
    for d in ways:
        for which in halves(d):
            if (d, which) not in passed:
                weights_from(d, which).wait_recv()

    span = wout.shape[2]

    def give(f):
        return pltpu.make_async_remote_copy(
            part_out.at[f],
            part_in.at[0, :, pl.ds(pl.multiple_of(f * span, span), span)],
            out_send.at[f],
            out_recv.at[f],
            device_id={"tp": other},
            device_id_type=MESH,
        )

    def columns(f, carry):
        theirs = act[pl.ds(pl.multiple_of(other * half, half), half), :]
        part_out[f] = jnp.dot(theirs, wout[f], preferred_element_type=jnp.float32).astype(
            jnp.bfloat16
        )
        give(f).start()
        mine = act[pl.ds(pl.multiple_of(tp * half, half), half), :]
        own[0, :, pl.ds(pl.multiple_of(f * span, span), span)] = jnp.dot(
            mine, wout[f], preferred_element_type=jnp.float32
        )
        return carry

    lax.fori_loop(0, n_fs, columns, 0)
    for f in range(n_fs):
        give(f).wait_recv()

    def sent(s, carry):
        to_pair(s).wait_send()

        @pl.when(sp < n_sp - 1)
        def _():
            to_right(s).wait_send()

        return carry

    lax.fori_loop(0, sp + 1, sent, 0)

    @pl.when(sp < n_sp - 1)
    def _():
        halo_copy.wait_send()

    stat_copy.wait_send()
    for d in ways:
        for which in halves(d):
            weights_pass(d, which).wait_send()
    for f in range(n_fs):
        give(f).wait_send()


def body(
    n_sp,
    n_fs,
    inputs,
    norm_gain,
    w_glu_value,
    w_glu_gate,
    w_query_one,
    w_query_two,
    w_key_one,
    w_key_two,
    w_value,
    conv_kernel,
    conv_gain,
    head_gain,
    lambda_head,
    w_out_conv,
    w_out_attn,
):
    half, model = inputs.shape[1:]
    rows = 2 * half
    width = w_glu_value.shape[1]
    t_glu = width // TILE
    t_qk = w_query_one.shape[1] // TILE
    t_v = w_value.shape[1] // TILE
    n_tiles = 2 * t_glu + 4 * t_qk + t_v
    heads = w_query_one.shape[1] // HD
    lanes = width // 128
    depth, span = w_out_conv.shape
    reach = -(-(conv_kernel.shape[0] - 1) // 16) * 16
    hbm = pl.BlockSpec(memory_space=pl.ANY)
    vmem = pl.BlockSpec(memory_space=pltpu.VMEM)
    f32, bf16 = jnp.float32, jnp.bfloat16
    dma = pltpu.SemaphoreType.DMA
    own, part, row_max, row_sum = pl.pallas_call(
        functools.partial(kernel, n_sp, n_fs, (t_glu, t_qk), 2 * width),
        out_shape=(
            jax.ShapeDtypeStruct((1, half, model), f32),
            jax.ShapeDtypeStruct((1, half, model), bf16),
            jax.ShapeDtypeStruct((1, 2, heads, rows), f32),
            jax.ShapeDtypeStruct((1, 2, heads, rows), f32),
        ),
        in_specs=[hbm] * 10 + [vmem] * 4 + [pl.BlockSpec(memory_space=pltpu.SMEM)],
        out_specs=(vmem, vmem, vmem, vmem),
        scratch_shapes=[
            pltpu.VMEM((half, model), bf16),
            pltpu.VMEM((n_sp, 2, half, model), bf16),
            pltpu.VMEM((n_tiles, model, TILE), bf16),
            pltpu.VMEM((n_fs, 2 * depth, span), bf16),
            pltpu.VMEM((n_tiles, rows, TILE), bf16),
            pltpu.VMEM((rows, width), bf16),
            pltpu.VMEM((reach, width), bf16),
            pltpu.VMEM((lanes, reach + rows, 128), f32),
            pltpu.VMEM((lanes, reach, 128), f32),
            pltpu.VMEM((lanes, rows, 128), f32),
            pltpu.VMEM((rows, 128), f32),
            pltpu.VMEM((rows, 128), f32),
            pltpu.VMEM((2 * heads, rows, 128), bf16),
            pltpu.VMEM((rows, rows), f32),
            pltpu.VMEM((2 * heads, VD, rows), f32),
            pltpu.VMEM((2 * heads, rows), f32),
            pltpu.VMEM((2 * heads, rows), f32),
            pltpu.VMEM((rows, width + heads * VD), bf16),
            pltpu.VMEM((n_fs, half, span), bf16),
            dma,
            dma((n_tiles,)),
            dma((2,)),
            dma((2 * n_fs, 2)),
            dma((n_fs, 2)),
            dma((n_sp,)),
            dma((n_sp,)),
            dma((n_sp,)),
            dma((n_sp,)),
            dma,
            dma,
            dma,
            dma,
            dma((n_fs,)),
            dma((n_fs,)),
        ],
        compiler_params=pltpu.CompilerParams(
            collective_id=0, has_side_effects=True, vmem_limit_bytes=63 * 1024 * 1024
        ),
        name="layer",
    )(
        inputs,
        w_glu_value,
        w_glu_gate,
        w_query_one,
        w_query_two,
        w_key_one,
        w_key_two,
        w_value,
        w_out_conv,
        w_out_attn,
        norm_gain.reshape(1, model),
        conv_kernel,
        conv_gain.reshape(1, width),
        head_gain.reshape(1, VD),
        lambda_head,
    )
    mixed = (own + part.astype(f32)).astype(bf16)
    return mixed, row_max + jnp.log(row_sum)


def solution(mesh):
    return jax.shard_map(
        functools.partial(body, mesh.shape["sp"], mesh.shape["fs"]),
        mesh=mesh,
        in_specs=(
            P("fs", ("sp", "tp"), None),
            P(),
            P(None, "tp"),
            P(None, "tp"),
            P(None, "tp"),
            P(None, "tp"),
            P(None, "tp"),
            P(None, "tp"),
            P(None, "tp"),
            P(None, "tp"),
            P("tp"),
            P(),
            P("tp"),
            P("tp", "fs"),
            P("tp", "fs"),
        ),
        out_specs=(P("fs", ("sp", "tp"), None), P("fs", None, "tp", "sp")),
        check_vma=False,
    )
```

```python
import functools

import jax
import jax.numpy as jnp
from jax import lax
from jax.experimental import pallas as pl
from jax.experimental.pallas import tpu as pltpu
from jax.sharding import PartitionSpec as P

HD = 64
VD = 128
SEG = 64
TILE = 256

NEG_FILL = -1e30
EPSILON = 1e-05
HEAD_SCALE = 0.8
MESH = pl.DeviceIdType.MESH


def kernel(
    n_sp,
    n_fs,
    tiles,
    channels,
    x_hbm,
    wgv,
    wgg,
    wq1,
    wq2,
    wk1,
    wk2,
    wv,
    woc,
    woa,
    norm_gain,
    conv_kernel,
    conv_gain,
    head_gain,
    lambda_head,
    own,
    part_in,
    max_out,
    sum_out,
    xb,
    nb,
    wall,
    wout,
    pbuf,
    gbuf,
    halo,
    ext,
    taps,
    cbuf,
    stat,
    stat_in,
    qm,
    bias,
    acc,
    m_sc,
    l_sc,
    act,
    part_out,
    x_sem,
    w_sem,
    wl_sem,
    wo_send,
    wo_recv,
    right_send,
    left_recv,
    pair_send,
    pair_recv,
    halo_send,
    halo_recv,
    stat_send,
    stat_recv,
    out_send,
    out_recv,
):
    sp = lax.axis_index("sp")
    fs = lax.axis_index("fs")
    tp = lax.axis_index("tp")
    other = 1 - tp
    half = xb.shape[0]
    rows = 2 * half
    t_glu, t_qk = tiles
    conv_tiles = t_glu
    base_q1 = 2 * t_glu
    base_q2 = base_q1 + t_qk
    base_k1 = base_q2 + t_qk
    base_k2 = base_k1 + t_qk
    base_v = base_k2 + t_qk
    n_tiles = wall.shape[0]
    heads = t_qk * TILE // HD
    width = wgv.shape[1]
    lanes = width // 128

    x_copy = pltpu.make_async_copy(x_hbm.at[0], xb, x_sem)
    x_copy.start()
    w_copies = []
    for ref, base, count in (
        (wgv, 0, t_glu),
        (wgg, t_glu, t_glu),
        (wq1, base_q1, t_qk),
        (wq2, base_q2, t_qk),
        (wk1, base_k1, t_qk),
        (wk2, base_k2, t_qk),
        (wv, base_v, n_tiles - base_v),
    ):
        for t in range(count):
            copy = pltpu.make_async_copy(
                ref.at[:, pl.ds(t * TILE, TILE)], wall.at[base + t], w_sem.at[base + t]
            )
            w_copies.append(copy)
    depth = woc.shape[0]
    wo_local = [
        pltpu.make_async_copy(ref, wout.at[fs, pl.ds(which * depth, depth)], wl_sem.at[which])
        for which, ref in enumerate((woc, woa))
    ]

    barrier = pltpu.get_barrier_semaphore()

    def greet(**where):
        pl.semaphore_signal(barrier, inc=1, device_id=where, device_id_type=MESH)

    greet(tp=other)
    for d in range(1, n_fs):
        greet(fs=lax.rem(fs + d, n_fs))

    @pl.when(sp > 0)
    def _():
        greet(sp=sp - 1)

    @pl.when(sp < n_sp - 1)
    def _():
        greet(sp=sp + 1)

    x_copy.wait()
    for copy in w_copies:
        copy.start()
    gain = norm_gain[...]

    def norm_rows(r, carry):
        at = pl.ds(pl.multiple_of(r * 16, 16), 16)
        x = xb[at, :].astype(jnp.float32)
        scale = lax.rsqrt(jnp.mean(x * x, axis=-1, keepdims=True) + EPSILON)
        nb[0, tp, at, :] = (x * scale * gain).astype(jnp.bfloat16)
        return carry

    lax.fori_loop(0, half // 16, norm_rows, 0, unroll=True)

    at_end = (sp == 0) | (sp == n_sp - 1)

    @pl.when(at_end)
    def _():
        pl.semaphore_wait(barrier, n_fs + 1)

    @pl.when(jnp.logical_not(at_end))
    def _():
        pl.semaphore_wait(barrier, n_fs + 2)

    def to_right(s):
        return pltpu.make_async_remote_copy(
            nb.at[s, tp],
            nb.at[s + 1, tp],
            right_send.at[s],
            left_recv.at[s + 1],
            device_id={"sp": lax.rem(sp + 1, n_sp)},
            device_id_type=MESH,
        )

    def to_pair(s):
        return pltpu.make_async_remote_copy(
            nb.at[s, tp],
            nb.at[s, tp],
            pair_send.at[s],
            pair_recv.at[s],
            device_id={"tp": other},
            device_id_type=MESH,
        )

    def from_pair(s):
        return pltpu.make_async_remote_copy(
            nb.at[s, other],
            nb.at[s, other],
            pair_send.at[s],
            pair_recv.at[s],
            device_id={"tp": other},
            device_id_type=MESH,
        )

    def place(index):
        if n_fs % 2:
            return index
        pair = index // 2
        return pair * 2 + lax.rem(lax.rem(index, 2) + pair, 2)

    seat = place(fs)

    def owner(d):
        return place(lax.rem(seat + n_fs + d, n_fs))

    def halves(d):
        if 2 * abs(d) < n_fs:
            return (0, 1) if d > 0 else (1, 0)
        if 2 * abs(d) == n_fs:
            return (0,) if d > 0 else (1,)
        return ()

    def weights_pass(d, which):
        sign = 1 if d > 0 else -1
        source = owner(-(d - sign))
        there = wout.at[source, pl.ds(which * depth, depth)]
        return pltpu.make_async_remote_copy(
            (woc, woa)[which] if abs(d) == 1 else there,
            there,
            wo_send.at[d + n_fs, which],
            wo_recv.at[source, which],
            device_id={"fs": owner(sign)},
            device_id_type=MESH,
        )

    def weights_from(d, which):
        source = owner(-d)
        there = wout.at[source, pl.ds(which * depth, depth)]
        return pltpu.make_async_remote_copy(
            there,
            there,
            wo_send.at[d + n_fs, which],
            wo_recv.at[source, which],
            device_id={"fs": source},
            device_id_type=MESH,
        )

    ways = [d for m in range(1, n_fs // 2 + 1) for d in (m, -m)]

    @pl.when(sp < n_sp - 1)
    def _():
        to_right(0).start()

    to_pair(0).start()

    for which in range(2):
        for d in ways[:2]:
            if which < len(halves(d)):
                weights_pass(d, halves(d)[which]).start()
    for copy in wo_local:
        copy.start()

    key_seg = lax.broadcasted_iota(jnp.int32, (rows, rows), 0) // SEG
    query_seg = lax.broadcasted_iota(jnp.int32, (rows, rows), 1) // SEG
    bias[...] = jnp.where(key_seg <= query_seg, 0.0, NEG_FILL)
    m_sc[...] = jnp.full(m_sc.shape, NEG_FILL, jnp.float32)
    l_sc[...] = jnp.zeros(l_sc.shape, jnp.float32)
    acc[...] = jnp.zeros(acc.shape, jnp.float32)
    n_taps = conv_kernel.shape[0]
    taps_f = conv_kernel[...].astype(jnp.float32)
    for c in range(lanes):
        taps[c, 0:n_taps, :] = taps_f[:, c * 128 : (c + 1) * 128]

    from_pair(0).wait_recv()

    def project(s, t):
        block = nb[s].reshape(rows, nb.shape[3])
        pbuf[t] = jnp.dot(block, wall[t], preferred_element_type=jnp.float32).astype(jnp.bfloat16)

    def first_project(t, carry):
        pltpu.make_async_copy(
            wgv.at[:, pl.ds(0, TILE)], wall.at[t], w_sem.at[t]
        ).wait()
        project(0, t)
        return carry

    lax.fori_loop(0, base_q1, first_project, 0)
    for t in range(conv_tiles):
        value = pbuf[t].astype(jnp.float32)
        gate = pbuf[conv_tiles + t].astype(jnp.float32)
        gbuf[:, t * TILE : (t + 1) * TILE] = (value * jax.nn.sigmoid(gate)).astype(jnp.bfloat16)
    reach = halo.shape[0]
    halo_copy = pltpu.make_async_remote_copy(
        gbuf.at[pl.ds(rows - reach, reach)],
        halo,
        halo_send,
        halo_recv,
        device_id={"sp": lax.rem(sp + 1, n_sp)},
        device_id_type=MESH,
    )

    @pl.when(sp < n_sp - 1)
    def _():
        halo_copy.start()

    lax.fori_loop(base_q1, n_tiles, first_project, 0)
    lane = lax.broadcasted_iota(jnp.int32, (rows, 128), 1)
    for i, base in enumerate((base_q1, base_q2)):
        for h in range(heads):
            tile, start = divmod(h * HD, TILE)
            start = start // 128 * 128
            queries = pbuf[base + tile, :, start : start + 128].astype(jnp.float32)
            inside = (lane // HD) == (h * HD % 128) // HD
            qm[i * heads + h] = jnp.where(inside, queries * HD**-0.5, 0.0).astype(jnp.bfloat16)

    for c in range(lanes):
        ext[c, reach:, :] = gbuf[:, c * 128 : (c + 1) * 128].astype(jnp.float32)

    @pl.when(sp == 0)
    def _():
        halo[...] = jnp.zeros(halo.shape, halo.dtype)

    @pl.when(sp > 0)
    def _():
        halo_copy.wait_recv()

    for c in range(lanes):
        ext[c, 0:reach, :] = halo[:, c * 128 : (c + 1) * 128].astype(jnp.float32)

    def conv_lanes(c, carry):
        sums, squares = carry
        lead = reach - (n_taps - 1)
        total = jnp.zeros((rows, 128), jnp.float32)
        for j in range(n_taps):
            total = total + taps[c, j : j + 1, :] * ext[c, lead + j : lead + j + rows, :]
        cbuf[c] = total
        return sums + total, squares + total * total

    zero = jnp.zeros((rows, 128), jnp.float32)
    sums, squares = lax.fori_loop(0, lanes, conv_lanes, (zero, zero))
    stat[...] = jnp.where(
        lane == 0,
        jnp.sum(sums, axis=-1, keepdims=True),
        jnp.sum(squares, axis=-1, keepdims=True),
    )
    stat_copy = pltpu.make_async_remote_copy(
        stat, stat_in, stat_send, stat_recv, device_id={"tp": other}, device_id_type=MESH
    )
    stat_copy.start()

    def take_next(s):
        to_right(s).wait_recv()

        @pl.when(sp < n_sp - 1)
        def _():
            to_right(s + 1).start()

        to_pair(s + 1).start()

    def step(s, carry):
        @pl.when((sp < n_sp - 1) & (s < sp))
        def _():
            take_next(s)

        @pl.when(s > 0)
        def _():
            from_pair(s).wait_recv()

            def again(t, inner):
                project(s, t)
                return inner

            lax.fori_loop(base_k1, n_tiles, again, 0, unroll=True)

            @pl.when(s == 1)
            def _():
                bias[...] = jnp.zeros(bias.shape, jnp.float32)

        for h in range(heads):
            v_tile, v_start = divmod(h * VD, TILE)
            values = pbuf[base_v + v_tile, :, v_start : v_start + VD]
            tile, start = divmod(h * HD, TILE)
            start = start // 128 * 128
            for i, base in enumerate((base_k1, base_k2)):
                c = i * heads + h
                keys = pbuf[base + tile, :, start : start + 128]
                scores = lax.dot_general(
                    keys, qm[c], (((1,), (1,)), ((), ())), preferred_element_type=jnp.float32
                )
                scores = scores + bias[...]
                old = m_sc[c : c + 1, :]
                new = jnp.maximum(old, jnp.max(scores, axis=0, keepdims=True))
                weights = jnp.exp(scores - new)
                factor = jnp.exp(old - new)
                m_sc[c : c + 1, :] = new
                l_sc[c : c + 1, :] = l_sc[c : c + 1, :] * factor + jnp.sum(
                    weights, axis=0, keepdims=True
                )
                acc[c] = acc[c] * factor + lax.dot_general(
                    values,
                    weights.astype(jnp.bfloat16),
                    (((0,), (0,)), ((), ())),
                    preferred_element_type=jnp.float32,
                )

        @pl.when(s == 0)
        def _():
            for d in ways[2:]:
                for which in halves(d):
                    weights_from(d - (1 if d > 0 else -1), which).wait_recv()
                    weights_pass(d, which).start()

        @pl.when((sp == n_sp - 1) & (s < sp))
        def _():
            take_next(s)

        return carry

    stat_copy.wait_recv()
    both = stat[...] + stat_in[...]
    row_mean = both[:, 0:1] / channels
    row_square = both[:, 1:2] / channels
    row_scale = lax.rsqrt(row_square - row_mean * row_mean + EPSILON)
    for c in range(lanes):
        at = slice(c * 128, (c + 1) * 128)
        z = (cbuf[c] - row_mean) * row_scale * conv_gain[:, at]
        act[:, at] = jax.nn.silu(z).astype(jnp.bfloat16)

    lax.fori_loop(0, sp + 1, step, 0)

    for i in range(2):
        max_out[0, i] = m_sc[i * heads : (i + 1) * heads, :]
        sum_out[0, i] = l_sc[i * heads : (i + 1) * heads, :]
    for h in range(heads):
        one = acc[h] / l_sc[h : h + 1, :]
        two = acc[heads + h] / l_sc[heads + h : heads + h + 1, :]
        head_out = one - lambda_head[h] * two
        head_out = head_out * lax.rsqrt(
            jnp.mean(head_out * head_out, axis=0, keepdims=True) + EPSILON
        )
        head_out = head_out.T * head_gain[...] * HEAD_SCALE
        act[:, width + h * VD : width + (h + 1) * VD] = head_out.astype(jnp.bfloat16)

    for copy in wo_local:
        copy.wait()
    passed = [(d - (1 if d > 0 else -1), which) for d in ways[2:] for which in halves(d)]
    for d in ways:
        for which in halves(d):
            if (d, which) not in passed:
                weights_from(d, which).wait_recv()

    span = wout.shape[2]

    def give(f):
        return pltpu.make_async_remote_copy(
            part_out.at[f],
            part_in.at[0, :, pl.ds(pl.multiple_of(f * span, span), span)],
            out_send.at[f],
            out_recv.at[f],
            device_id={"tp": other},
            device_id_type=MESH,
        )

    def columns(f, carry):
        theirs = act[pl.ds(pl.multiple_of(other * half, half), half), :]
        part_out[f] = jnp.dot(theirs, wout[f], preferred_element_type=jnp.float32).astype(
            jnp.bfloat16
        )
        give(f).start()
        mine = act[pl.ds(pl.multiple_of(tp * half, half), half), :]
        own[0, :, pl.ds(pl.multiple_of(f * span, span), span)] = jnp.dot(
            mine, wout[f], preferred_element_type=jnp.float32
        )
        return carry

    lax.fori_loop(0, n_fs, columns, 0, unroll=True)
    for f in range(n_fs):
        give(f).wait_recv()

    def sent(s, carry):
        to_pair(s).wait_send()

        @pl.when(sp < n_sp - 1)
        def _():
            to_right(s).wait_send()

        return carry

    lax.fori_loop(0, sp + 1, sent, 0)

    @pl.when(sp < n_sp - 1)
    def _():
        halo_copy.wait_send()

    stat_copy.wait_send()
    for d in ways:
        for which in halves(d):
            weights_pass(d, which).wait_send()
    for f in range(n_fs):
        give(f).wait_send()


def finish(own, part, row_max, row_sum, mixed, logs):
    mixed[...] = (own[...] + part[...].astype(jnp.float32)).astype(jnp.bfloat16)
    logs[...] = row_max[...] + jnp.log(row_sum[...])


def body(
    n_sp,
    n_fs,
    inputs,
    norm_gain,
    w_glu_value,
    w_glu_gate,
    w_query_one,
    w_query_two,
    w_key_one,
    w_key_two,
    w_value,
    conv_kernel,
    conv_gain,
    head_gain,
    lambda_head,
    w_out_conv,
    w_out_attn,
):
    half, model = inputs.shape[1:]
    rows = 2 * half
    width = w_glu_value.shape[1]
    t_glu = width // TILE
    t_qk = w_query_one.shape[1] // TILE
    t_v = w_value.shape[1] // TILE
    n_tiles = 2 * t_glu + 4 * t_qk + t_v
    heads = w_query_one.shape[1] // HD
    lanes = width // 128
    depth, span = w_out_conv.shape
    reach = -(-(conv_kernel.shape[0] - 1) // 16) * 16
    hbm = pl.BlockSpec(memory_space=pl.ANY)
    vmem = pl.BlockSpec(memory_space=pltpu.VMEM)
    f32, bf16 = jnp.float32, jnp.bfloat16
    dma = pltpu.SemaphoreType.DMA
    own, part, row_max, row_sum = pl.pallas_call(
        functools.partial(kernel, n_sp, n_fs, (t_glu, t_qk), 2 * width),
        out_shape=(
            jax.ShapeDtypeStruct((1, half, model), f32),
            jax.ShapeDtypeStruct((1, half, model), bf16),
            jax.ShapeDtypeStruct((1, 2, heads, rows), f32),
            jax.ShapeDtypeStruct((1, 2, heads, rows), f32),
        ),
        in_specs=[hbm] * 10 + [vmem] * 4 + [pl.BlockSpec(memory_space=pltpu.SMEM)],
        out_specs=(vmem, vmem, vmem, vmem),
        scratch_shapes=[
            pltpu.VMEM((half, model), bf16),
            pltpu.VMEM((n_sp, 2, half, model), bf16),
            pltpu.VMEM((n_tiles, model, TILE), bf16),
            pltpu.VMEM((n_fs, 2 * depth, span), bf16),
            pltpu.VMEM((n_tiles, rows, TILE), bf16),
            pltpu.VMEM((rows, width), bf16),
            pltpu.VMEM((reach, width), bf16),
            pltpu.VMEM((lanes, reach + rows, 128), f32),
            pltpu.VMEM((lanes, reach, 128), f32),
            pltpu.VMEM((lanes, rows, 128), f32),
            pltpu.VMEM((rows, 128), f32),
            pltpu.VMEM((rows, 128), f32),
            pltpu.VMEM((2 * heads, rows, 128), bf16),
            pltpu.VMEM((rows, rows), f32),
            pltpu.VMEM((2 * heads, VD, rows), f32),
            pltpu.VMEM((2 * heads, rows), f32),
            pltpu.VMEM((2 * heads, rows), f32),
            pltpu.VMEM((rows, width + heads * VD), bf16),
            pltpu.VMEM((n_fs, half, span), bf16),
            dma,
            dma((n_tiles,)),
            dma((2,)),
            dma((2 * n_fs, 2)),
            dma((n_fs, 2)),
            dma((n_sp,)),
            dma((n_sp,)),
            dma((n_sp,)),
            dma((n_sp,)),
            dma,
            dma,
            dma,
            dma,
            dma((n_fs,)),
            dma((n_fs,)),
        ],
        compiler_params=pltpu.CompilerParams(
            collective_id=0, has_side_effects=True, vmem_limit_bytes=63 * 1024 * 1024
        ),
        name="layer",
    )(
        inputs,
        w_glu_value,
        w_glu_gate,
        w_query_one,
        w_query_two,
        w_key_one,
        w_key_two,
        w_value,
        w_out_conv,
        w_out_attn,
        norm_gain.reshape(1, model),
        conv_kernel,
        conv_gain.reshape(1, width),
        head_gain.reshape(1, VD),
        lambda_head,
    )
    return pl.pallas_call(
        finish,
        out_shape=(
            jax.ShapeDtypeStruct((1, half, model), bf16),
            jax.ShapeDtypeStruct((1, 2, heads, rows), f32),
        ),
        in_specs=[vmem] * 4,
        out_specs=(vmem, vmem),
        name="finish",
    )(own, part, row_max, row_sum)


def solution(mesh):
    return jax.shard_map(
        functools.partial(body, mesh.shape["sp"], mesh.shape["fs"]),
        mesh=mesh,
        in_specs=(
            P("fs", ("sp", "tp"), None),
            P(),
            P(None, "tp"),
            P(None, "tp"),
            P(None, "tp"),
            P(None, "tp"),
            P(None, "tp"),
            P(None, "tp"),
            P(None, "tp"),
            P(None, "tp"),
            P("tp"),
            P(),
            P("tp"),
            P("tp", "fs"),
            P("tp", "fs"),
        ),
        out_specs=(P("fs", ("sp", "tp"), None), P("fs", None, "tp", "sp")),
        check_vma=False,
    )
```
